256 devices in a mesh: grp: 2 (over y), ra: 16 (over z), cb: 8 (over x, core).
Axes of the slice: x: 4, y: 2, z: 16, core: 2. Of those that a mesh axis runs over, the one named last changes fastest.
The devices are a block of a 4x16x16 slice.
Arguments:
- tokens: bfloat16 [256, 2048], P('grp', 'ra'), parts along dimension 0, may hold values from -8 to 8
- first_gain: bfloat16 [2048], P('ra'), may hold values from 0.099609375 to 1.8984375
- first_gate: bfloat16 [2048, 5632], P('ra', 'cb'), may hold values from -0.125 to 0.125
- first_up: bfloat16 [2048, 5632], P('ra', 'cb'), may hold values from -0.125 to 0.125
- first_down: bfloat16 [5632, 2048], P('cb', 'ra'), may hold values from -0.078125 to 0.078125
- second_gain: bfloat16 [2048], P('ra'), may hold values from 0.099609375 to 1.8984375
- second_gate: bfloat16 [2048, 5632], P('ra', 'cb'), may hold values from -0.125 to 0.125
- second_up: bfloat16 [2048, 5632], P('ra', 'cb'), may hold values from -0.125 to 0.125
- second_down: bfloat16 [5632, 2048], P('cb', 'ra'), may hold values from -0.078125 to 0.078125
Outputs:
- latent_out: bfloat16 [256, 2048], P('grp', 'ra'), parts along dimension 0
The draws below stay inside these ranges and needn't reach their ends.
There are 2 independent parts, one for each index of `grp`. The reference program is written for one: setup_inputs(seed, part) draws one part's arguments, and reference() takes and returns one part's arrays. A program takes and returns all parts, laid end to end along the dimension named above; an argument that names none is the same for every part. Nothing has to cross between parts.
All inputs are finite; a program needn't handle non-finite values.
Results may differ from the reference program's by a relative error of at most 0.0088.
Values may be sent and summed in bfloat16 or wider, within the bound.
A program may use at most 64 MiB of HBM per device.

```python
import math
import jax
import jax.numpy as jnp
from jax import lax

D = 2048
FF = 5632
TOKENS = 128


def draw_tokens(key, part):
    keys = jax.random.split(jax.random.fold_in(key, 11), 3)
    row_scale = jnp.exp(jax.random.uniform(keys[0], (TOKENS, 1), jnp.float32, math.log(0.1), 0.0))
    ramp = jnp.exp(math.log(6.0) * jnp.arange(D, dtype=jnp.float32) / D) / 2.5
    col_scale = ramp * jnp.exp(jax.random.uniform(keys[1], (D,), jnp.float32, -0.35, 0.35))
    base = jax.random.normal(keys[2], (TOKENS, D), jnp.float32)
    return jnp.clip(base * row_scale * col_scale, -8.0, 8.0).astype(jnp.bfloat16)


def steps_of(rng, dims, cuts, smallest, largest):
    def one(axis_at, shards_of):
        heights = jax.random.uniform(jax.random.fold_in(jax.random.fold_in(rng, 6), axis_at), (shards_of,), jnp.float32, smallest / len(cuts), largest / len(cuts))
        return jnp.repeat(jnp.exp(heights), dims[axis_at] // shards_of).reshape((-1,) + (1,) * (len(dims) - axis_at - 1))

    factor_of = one(*cuts[0])
    for cut in cuts[1:]:
        factor_of = factor_of * one(*cut)
    return factor_of


def centred(key, extent, deviation, bound, shards=(), kind=jnp.bfloat16):
    level = steps_of(key, extent, shards, -0.22, 0.18) if shards else 1.0
    result = jax.random.normal(key, extent, jnp.float32) * deviation * level
    return jnp.minimum(jnp.maximum(result, -bound), bound).astype(kind)


def setup_inputs(seed: int = 0, part: int = 0) -> dict:
    key_of = jax.random.split(jax.random.key(seed), 10)
    part_keys = jax.random.split(jax.random.fold_in(key_of[9], part), 10)
    tokens = draw_tokens(jax.random.fold_in(jax.random.fold_in(key_of[9], part), 71), part)
    first_gain = jnp.clip(1.0 + 0.18 * jax.random.normal(key_of[1], (D,), jnp.float32), 0.099609375, 1.8984375).astype(jnp.bfloat16)
    first_gate = centred(key_of[2], (D, FF), D ** -0.5, 0.125, ((0, 16), (1, 8)))
    first_up = centred(key_of[3], (D, FF), D ** -0.5, 0.125, ((0, 16), (1, 8)))
    first_down = centred(key_of[4], (FF, D), FF ** -0.5, 0.078125, ((0, 8), (1, 16)))
    second_gain = jnp.clip(1.0 + 0.18 * jax.random.normal(key_of[5], (D,), jnp.float32), 0.099609375, 1.8984375).astype(jnp.bfloat16)
    second_gate = centred(key_of[6], (D, FF), D ** -0.5, 0.125, ((0, 16), (1, 8)))
    second_up = centred(key_of[7], (D, FF), D ** -0.5, 0.125, ((0, 16), (1, 8)))
    second_down = centred(key_of[8], (FF, D), FF ** -0.5, 0.078125, ((0, 8), (1, 16)))
    return {"tokens": tokens, "first_gain": first_gain, "first_gate": first_gate, "first_up": first_up, "first_down": first_down, "second_gain": second_gain, "second_gate": second_gate, "second_up": second_up, "second_down": second_down}


def sublayer(x, gain, w_gate, w_up, w_down):
    xf = x.astype(jnp.float32)
    scale = jax.lax.rsqrt(lax.optimization_barrier(jnp.mean(xf * xf, axis=1)) + 1e-06)
    normed = (xf * gain.astype(jnp.float32)).astype(jnp.bfloat16)
    gate_pre = scale[:, None] * jnp.dot(normed, w_gate, preferred_element_type=jnp.float32)
    up_pre = scale[:, None] * jnp.dot(normed, w_up, preferred_element_type=jnp.float32)
    hidden = (jax.nn.silu(gate_pre) * up_pre).astype(jnp.bfloat16)
    branch = jnp.dot(hidden, w_down, preferred_element_type=jnp.float32)
    return (0.5 * xf + 0.5 * branch).astype(jnp.bfloat16)

def reference(tokens, first_gain, first_gate, first_up, first_down, second_gain, second_gate, second_up, second_down):
    middle = sublayer(tokens, first_gain, first_gate, first_up, first_down)
    return sublayer(middle, second_gain, second_gate, second_up, second_down)
```

```python
import functools

import jax
import jax.numpy as jnp
from jax import lax
from jax.experimental import pallas as pl
from jax.experimental.pallas import tpu as pltpu
from jax.sharding import PartitionSpec as P

MESH = pl.DeviceIdType.MESH
LANES = 128
BF16 = jnp.bfloat16
F32 = jnp.float32


def far_first(n):
    return sorted(range(1, n), key=lambda o: -min(o, n - o))


def fused(n_ra, n_cb, tokens, gain1, gate1, up1, down1, gain2, gate2, up2, down2, out,
          x_v, gain_v, gate_v, up_v, down_v, x_f,
          rs_out, rs_in, ag_out, ag_in, ar_in,
          load_sem, rs_send, rs_recv, ag_send, ag_recv, ar_send, ar_recv):
    ra = lax.axis_index("ra")
    cb = lax.axis_index("cb")
    rows, cols = x_v.shape
    oct_rows = rows // n_ra
    units = gate_v.shape[2]
    half = rs_in.shape[3] // 2
    width = cols * n_ra

    loads = [pltpu.make_async_copy(tokens, x_v, load_sem.at[0])]
    for s, (gn, gt, up, dn) in enumerate(((gain1, gate1, up1, down1), (gain2, gate2, up2, down2))):
        loads += [
            pltpu.make_async_copy(gn, gain_v.at[s], load_sem.at[4 * s + 1]),
            pltpu.make_async_copy(gt, gate_v.at[s], load_sem.at[4 * s + 2]),
            pltpu.make_async_copy(up, up_v.at[s], load_sem.at[4 * s + 3]),
            pltpu.make_async_copy(dn, down_v.at[s], load_sem.at[4 * s + 4]),
        ]
    for c in loads:
        c.start()

    barrier = pltpu.get_barrier_semaphore()
    for o in far_first(n_ra):
        pl.semaphore_signal(barrier, 1, device_id={"ra": lax.rem(ra + o, n_ra)}, device_id_type=MESH)
    for o in range(1, n_cb):
        pl.semaphore_signal(barrier, 1, device_id={"cb": lax.rem(cb + o, n_cb)}, device_id_type=MESH)

    for s in range(2):
        if s == 0:
            loads[0].wait()
            xf = x_v[...].astype(F32)
        else:
            xf = x_f[...]
        for c in loads[4 * s + 1:4 * s + 4]:
            c.wait()
        sq = jnp.sum(xf * xf, axis=1, keepdims=True)
        hi = sq.astype(BF16).astype(F32)
        normed = (xf * gain_v[s].astype(F32)).astype(BF16)
        pad = half - units
        for w, at, extra in ((gate_v, 0, hi), (up_v, half, sq - hi)):
            part = jnp.dot(normed, w[s], preferred_element_type=F32)
            rs_out[:, :, at:at + units] = part.reshape(n_ra, oct_rows, units).astype(BF16)
            rs_out[:, :, at + units:at + half] = jnp.broadcast_to(
                extra.reshape(n_ra, oct_rows, 1), (n_ra, oct_rows, pad)).astype(BF16)
        if s == 0:
            pl.semaphore_wait(barrier, n_ra - 1 + n_cb - 1)
        sends = []
        for o in far_first(n_ra):
            to = lax.rem(ra + o, n_ra)
            c = pltpu.make_async_remote_copy(
                src_ref=rs_out.at[to], dst_ref=rs_in.at[s, o], send_sem=rs_send.at[o],
                recv_sem=rs_recv.at[s, o], device_id={"ra": to}, device_id_type=MESH)
            c.start()
            sends.append(c)
        total = rs_out[ra].astype(F32)
        for o in reversed(far_first(n_ra)):
            pltpu.make_async_remote_copy(
                src_ref=rs_out.at[0], dst_ref=rs_in.at[s, o], send_sem=rs_send.at[o],
                recv_sem=rs_recv.at[s, o], device_id={"ra": ra}, device_id_type=MESH).wait_recv()
            total = total + rs_in[s, o].astype(F32)
        sumsq = total[:, units:units + 1] + total[:, half + units:half + units + 1]
        scale = lax.rsqrt(sumsq / width + 1e-06)
        g = total[:, :units] * scale
        hidden = (g / (1.0 + jnp.exp(-g)) * (total[:, half:half + units] * scale)).astype(BF16)
        ag_out[s] = hidden
        ag_in[s, ra] = hidden
        ag = []
        for o in far_first(n_ra):
            to = lax.rem(ra + o, n_ra)
            c = pltpu.make_async_remote_copy(
                src_ref=ag_out.at[s], dst_ref=ag_in.at[s, ra], send_sem=ag_send.at[o],
                recv_sem=ag_recv.at[s, o], device_id={"ra": to}, device_id_type=MESH)
            c.start()
            ag.append(c)
        loads[4 * s + 4].wait()
        for o in reversed(far_first(n_ra)):
            pltpu.make_async_remote_copy(
                src_ref=ag_out.at[s], dst_ref=ag_in.at[s, lax.rem(ra + n_ra - o, n_ra)], send_sem=ag_send.at[o],
                recv_sem=ag_recv.at[s, o], device_id={"ra": ra}, device_id_type=MESH).wait_recv()
        h = ag_in[s].astype(F32).reshape(rows, units).astype(BF16)
        ar_in[s, cb] = jnp.dot(h, down_v[s], preferred_element_type=F32).astype(BF16)
        ar = []
        for o in far_first(n_cb):
            c = pltpu.make_async_remote_copy(
                src_ref=ar_in.at[s, cb], dst_ref=ar_in.at[s, cb], send_sem=ar_send.at[o],
                recv_sem=ar_recv.at[s, o], device_id={"cb": lax.rem(cb + o, n_cb)}, device_id_type=MESH)
            c.start()
            ar.append(c)
        for o in reversed(far_first(n_cb)):
            pltpu.make_async_remote_copy(
                src_ref=ar_in.at[s, cb], dst_ref=ar_in.at[s, lax.rem(cb + n_cb - o, n_cb)], send_sem=ar_send.at[o],
                recv_sem=ar_recv.at[s, o], device_id={"cb": cb}, device_id_type=MESH).wait_recv()
        branch = ar_in[s, 0].astype(F32)
        for c in range(1, n_cb):
            branch = branch + ar_in[s, c].astype(F32)
        result = (0.5 * xf + 0.5 * branch).astype(BF16)
        if s == 0:
            x_f[...] = result.astype(F32)
        else:
            out[...] = result
        for c in sends + ag + ar:
            c.wait_send()


def per_device(tokens, first_gain, first_gate, first_up, first_down,
               second_gain, second_gate, second_up, second_down):
    n_ra, n_cb = lax.axis_size("ra"), lax.axis_size("cb")
    rows, cols = tokens.shape
    units = first_gate.shape[1]
    half = -(-units // LANES) * LANES
    if half == units:
        half += LANES
    o_rows = rows // n_ra
    dma = pltpu.SemaphoreType.DMA
    any_spec = pl.BlockSpec(memory_space=pl.ANY)
    return pl.pallas_call(
        functools.partial(fused, n_ra, n_cb),
        out_shape=jax.ShapeDtypeStruct((rows, cols), BF16),
        in_specs=[any_spec] * 9,
        out_specs=pl.BlockSpec(memory_space=pltpu.VMEM),
        scratch_shapes=[
            pltpu.VMEM((rows, cols), BF16),
            pltpu.VMEM((2, 1, cols), BF16),
            pltpu.VMEM((2, cols, units), BF16),
            pltpu.VMEM((2, cols, units), BF16),
            pltpu.VMEM((2, units, cols), BF16),
            pltpu.VMEM((rows, cols), F32),
            pltpu.VMEM((n_ra, o_rows, 2 * half), BF16),
            pltpu.VMEM((2, n_ra, o_rows, 2 * half), BF16),
            pltpu.VMEM((2, o_rows, units), BF16),
            pltpu.VMEM((2, n_ra, o_rows, units), BF16),
            pltpu.VMEM((2, n_cb, rows, cols), BF16),
            dma((9,)),
            dma((n_ra,)), dma((2, n_ra)),
            dma((n_ra,)), dma((2, n_ra)),
            dma((n_cb,)), dma((2, n_cb)),
        ],
        compiler_params=pltpu.CompilerParams(collective_id=0, has_side_effects=True),
    )(tokens, first_gain.reshape(1, -1), first_gate, first_up, first_down,
      second_gain.reshape(1, -1), second_gate, second_up, second_down)


def solution(mesh):
    placed = (
        P("grp", "ra"),
        P("ra"), P("ra", "cb"), P("ra", "cb"), P("cb", "ra"),
        P("ra"), P("ra", "cb"), P("ra", "cb"), P("cb", "ra"),
    )
    return jax.shard_map(
        per_device, mesh=mesh, in_specs=placed, out_specs=P("grp", "ra"), check_vma=False
    )
```

```python
import functools

import jax
import jax.numpy as jnp
from jax import lax
from jax.experimental import pallas as pl
from jax.experimental.pallas import tpu as pltpu
from jax.sharding import PartitionSpec as P

MESH = pl.DeviceIdType.MESH
LANES = 128
BF16 = jnp.bfloat16
F32 = jnp.float32


def far_first(n):
    return sorted(range(1, n), key=lambda o: -min(o, n - o))


def fused(n_ra, n_cb, tokens, gain1, gate1, up1, down1, gain2, gate2, up2, down2, out,
          x_v, gain_v, gate_v, up_v, down_v, x_f,
          rs_out, rs_in, ag_out, ag_in, ar_in,
          ready, load_sem, rs_send, rs_recv, ag_send, ag_recv, ar_send, ar_recv):
    ra = lax.axis_index("ra")
    cb = lax.axis_index("cb")
    rows, cols = x_v.shape
    oct_rows = rows // n_ra
    units = gate_v.shape[1]
    half = rs_in.shape[3] // 2
    width = cols * n_ra

    loads = [pltpu.make_async_copy(tokens, x_v, load_sem.at[0])]
    for s, (gn, gt, up, dn) in enumerate(((gain1, gate1, up1, down1), (gain2, gate2, up2, down2))):
        loads += [
            pltpu.make_async_copy(gn, gain_v.at[s], load_sem.at[4 * s + 1]),
            pltpu.make_async_copy(gt, gate_v.at[s], load_sem.at[4 * s + 2]),
            pltpu.make_async_copy(up, up_v.at[s], load_sem.at[4 * s + 3]),
            pltpu.make_async_copy(dn, down_v.at[s], load_sem.at[4 * s + 4]),
        ]
    for c in loads:
        c.start()

    barrier = pltpu.get_barrier_semaphore()
    for o in range(1, n_cb):
        pl.semaphore_signal(barrier, 1, device_id={"cb": lax.rem(cb + o, n_cb)}, device_id_type=MESH)
    pl.semaphore_wait(barrier, n_cb - 1 + jnp.where(ra > 0, 1, 0))

    @pl.when(ra < n_ra - 1)
    def _():
        pl.semaphore_signal(barrier, 1, device_id={"ra": ra + 1}, device_id_type=MESH)

    for o in far_first(n_ra):
        @pl.when(ra >= o)
        def _():
            pl.semaphore_signal(ready.at[o], 1, device_id={"ra": ra - o}, device_id_type=MESH)

    for s in range(2):
        if s == 0:
            loads[0].wait()
            xf = x_v[...].astype(F32)
        else:
            xf = x_f[...]
        for c in loads[4 * s + 1:4 * s + 4]:
            c.wait()
        sq = jnp.sum(xf * xf, axis=1, keepdims=True)
        hi = sq.astype(BF16).astype(F32)
        normed = (xf * gain_v[s].astype(F32)).astype(BF16)
        pad = half - units
        for w, at, extra in ((gate_v, 0, hi), (up_v, half, sq - hi)):
            part = lax.dot_general(normed, w[s], (((1,), (1,)), ((), ())), preferred_element_type=F32)
            rs_out[:, :, at:at + units] = part.reshape(n_ra, oct_rows, units).astype(BF16)
            rs_out[:, :, at + units:at + half] = jnp.broadcast_to(
                extra.reshape(n_ra, oct_rows, 1), (n_ra, oct_rows, pad)).astype(BF16)
        sends = []
        for o in far_first(n_ra):
            to = lax.rem(ra + o, n_ra)
            sends.append(pltpu.make_async_remote_copy(
                src_ref=rs_out.at[to], dst_ref=rs_in.at[s, o], send_sem=rs_send.at[o],
                recv_sem=rs_recv.at[s, o], device_id={"ra": to}, device_id_type=MESH))
        if s == 0:
            for o, c in zip(far_first(n_ra), sends):
                pl.when(ra + o >= n_ra)(c.start)
            for o, c in sorted(zip(far_first(n_ra), sends), key=lambda oc: oc[0]):
                @pl.when(ra + o < n_ra)
                def _():
                    pl.semaphore_wait(ready.at[o], 1)
                    c.start()
        else:
            for c in sends:
                c.start()
        total = rs_out[ra].astype(F32)
        for o in reversed(far_first(n_ra)):
            pltpu.make_async_remote_copy(
                src_ref=rs_out.at[0], dst_ref=rs_in.at[s, o], send_sem=rs_send.at[o],
                recv_sem=rs_recv.at[s, o], device_id={"ra": ra}, device_id_type=MESH).wait_recv()
            total = total + rs_in[s, o].astype(F32)
        sumsq = total[:, units:units + 1] + total[:, half + units:half + units + 1]
        scale = lax.rsqrt(sumsq / width + 1e-06)
        g = total[:, :units] * scale
        hidden = (g / (1.0 + jnp.exp(-g)) * (total[:, half:half + units] * scale)).astype(BF16)
        ag_out[s] = hidden
        ag_in[s, ra] = hidden
        ag = []
        for o in far_first(n_ra):
            to = lax.rem(ra + o, n_ra)
            c = pltpu.make_async_remote_copy(
                src_ref=ag_out.at[s], dst_ref=ag_in.at[s, ra], send_sem=ag_send.at[o],
                recv_sem=ag_recv.at[s, o], device_id={"ra": to}, device_id_type=MESH)
            c.start()
            ag.append(c)
        loads[4 * s + 4].wait()
        for o in reversed(far_first(n_ra)):
            pltpu.make_async_remote_copy(
                src_ref=ag_out.at[s], dst_ref=ag_in.at[s, lax.rem(ra + n_ra - o, n_ra)], send_sem=ag_send.at[o],
                recv_sem=ag_recv.at[s, o], device_id={"ra": ra}, device_id_type=MESH).wait_recv()
        h = ag_in[s].astype(F32).reshape(rows, units).astype(BF16)
        ar_in[s, cb] = jnp.dot(h, down_v[s], preferred_element_type=F32).astype(BF16)
        ar = []
        for o in far_first(n_cb):
            c = pltpu.make_async_remote_copy(
                src_ref=ar_in.at[s, cb], dst_ref=ar_in.at[s, cb], send_sem=ar_send.at[o],
                recv_sem=ar_recv.at[s, o], device_id={"cb": lax.rem(cb + o, n_cb)}, device_id_type=MESH)
            c.start()
            ar.append(c)
        for o in reversed(far_first(n_cb)):
            pltpu.make_async_remote_copy(
                src_ref=ar_in.at[s, cb], dst_ref=ar_in.at[s, lax.rem(cb + n_cb - o, n_cb)], send_sem=ar_send.at[o],
                recv_sem=ar_recv.at[s, o], device_id={"cb": cb}, device_id_type=MESH).wait_recv()
        branch = ar_in[s, 0].astype(F32)
        for c in range(1, n_cb):
            branch = branch + ar_in[s, c].astype(F32)
        result = (0.5 * xf + 0.5 * branch).astype(BF16)
        if s == 0:
            x_f[...] = result.astype(F32)
        else:
            out[...] = result
        for c in sends + ag + ar:
            c.wait_send()


def per_device(tokens, first_gain, first_gate, first_up, first_down,
               second_gain, second_gate, second_up, second_down):
    n_ra, n_cb = lax.axis_size("ra"), lax.axis_size("cb")
    rows, cols = tokens.shape
    units = first_gate.shape[1]
    half = -(-units // LANES) * LANES
    if half == units:
        half += LANES
    o_rows = rows // n_ra
    dma = pltpu.SemaphoreType.DMA
    any_spec = pl.BlockSpec(memory_space=pl.ANY)
    return pl.pallas_call(
        functools.partial(fused, n_ra, n_cb),
        out_shape=jax.ShapeDtypeStruct((rows, cols), BF16),
        in_specs=[any_spec] * 9,
        out_specs=pl.BlockSpec(memory_space=pltpu.VMEM),
        scratch_shapes=[
            pltpu.VMEM((rows, cols), BF16),
            pltpu.VMEM((2, 1, cols), BF16),
            pltpu.VMEM((2, units, cols), BF16),
            pltpu.VMEM((2, units, cols), BF16),
            pltpu.VMEM((2, units, cols), BF16),
            pltpu.VMEM((rows, cols), F32),
            pltpu.VMEM((n_ra, o_rows, 2 * half), BF16),
            pltpu.VMEM((2, n_ra, o_rows, 2 * half), BF16),
            pltpu.VMEM((2, o_rows, units), BF16),
            pltpu.VMEM((2, n_ra, o_rows, units), BF16),
            pltpu.VMEM((2, n_cb, rows, cols), BF16),
            pltpu.SemaphoreType.REGULAR((n_ra,)),
            dma((9,)),
            dma((n_ra,)), dma((2, n_ra)),
            dma((n_ra,)), dma((2, n_ra)),
            dma((n_cb,)), dma((2, n_cb)),
        ],
        compiler_params=pltpu.CompilerParams(collective_id=0, has_side_effects=True),
    )(tokens, first_gain.reshape(1, -1), first_gate.T, first_up.T, first_down,
      second_gain.reshape(1, -1), second_gate.T, second_up.T, second_down)


def solution(mesh):
    placed = (
        P("grp", "ra"),
        P("ra"), P("ra", "cb"), P("ra", "cb"), P("cb", "ra"),
        P("ra"), P("ra", "cb"), P("ra", "cb"), P("cb", "ra"),
    )
    return jax.shard_map(
        per_device, mesh=mesh, in_specs=placed, out_specs=P("grp", "ra"), check_vma=False
    )
```

```python
import functools

import jax
import jax.numpy as jnp
from jax import lax
from jax.experimental import pallas as pl
from jax.experimental.pallas import tpu as pltpu
from jax.sharding import PartitionSpec as P

MESH = pl.DeviceIdType.MESH
LANES = 128
BF16 = jnp.bfloat16
F32 = jnp.float32
scope = jax.named_scope
GROUPS = 4


def far_first(n):
    return sorted(range(1, n), key=lambda o: -min(o, n - o))


def groups_of(n):
    order = far_first(n) + [0]
    size = n // GROUPS
    return [order[i * size:(i + 1) * size] for i in range(GROUPS)]


def fused(n_ra, n_cb, tokens, gain1, gate1, up1, down1, gain2, gate2, up2, down2, out,
          x_v, gain_v, gate_v, up_v, down_v, x_f,
          rs_out, sums, rs_in, ag_out, ag_in, ar_in,
          ready, column, row, all_in, load_sem, rs_send, rs_recv, ag_send, ag_recv, ar_send, ar_recv):
    ra = lax.axis_index("ra")
    cb = lax.axis_index("cb")
    rows, cols = x_v.shape
    piece = rows // n_ra
    units = gate_v.shape[1]
    half = rs_in.shape[3] // 2
    width = cols * n_ra
    groups = groups_of(n_ra)

    hop = n_ra // 4
    ahead = list(range(hop + 1, n_ra // 2 + 1))
    behind = list(range(n_ra // 2 + 1, n_ra - hop))
    near = list(range(1, hop + 1)) + list(range(n_ra - hop, n_ra))

    def at(o):
        return lax.rem(ra + o, n_ra)

    loads = [pltpu.make_async_copy(tokens, x_v, load_sem.at[0])]
    for s, (gn, gt, up, dn) in enumerate(((gain1, gate1, up1, down1), (gain2, gate2, up2, down2))):
        loads += [
            pltpu.make_async_copy(gn, gain_v.at[s], load_sem.at[4 * s + 1]),
            pltpu.make_async_copy(gt, gate_v.at[s], load_sem.at[4 * s + 2]),
            pltpu.make_async_copy(up, up_v.at[s], load_sem.at[4 * s + 3]),
            pltpu.make_async_copy(dn, down_v.at[s], load_sem.at[4 * s + 4]),
        ]
    for c in loads:
        c.start()

    turn = at(n_ra - 1)
    barrier = pltpu.get_barrier_semaphore()

    @pl.when(turn == 0)
    def _():
        for o in range(1, n_cb):
            pl.semaphore_signal(barrier, 1, device_id={"cb": lax.rem(cb + o, n_cb)}, device_id_type=MESH)

    with scope("barrier"):
        pl.semaphore_wait(barrier, jnp.where(turn == 0, n_cb - 1, 1))

    @pl.when(turn < n_ra - 1)
    def _():
        pl.semaphore_signal(barrier, 1, device_id={"ra": at(1)}, device_id_type=MESH)

    for o in near:
        @pl.when(turn >= o)
        def _():
            pl.semaphore_signal(ready.at[o], 1, device_id={"ra": at(n_ra - o)}, device_id_type=MESH)

    @pl.when(turn > 0)
    def _():
        pl.semaphore_signal(column, 1, device_id={"ra": lax.rem(ra + n_ra - turn, n_ra)}, device_id_type=MESH)

    def project(s, xf, places):
        sq = jnp.sum(xf * xf, axis=1, keepdims=True)
        hi = sq.astype(BF16).astype(F32)
        normed = (xf * gain_v[s].astype(F32)).astype(BF16)
        for w, lane, extra in ((gate_v, 0, hi), (up_v, half, sq - hi)):
            part = lax.dot_general(normed, w[s], (((1,), (1,)), ((), ())), preferred_element_type=F32)
            for i, place in enumerate(places):
                cut = slice(i * piece, (i + 1) * piece)
                rs_out[s, place, :, lane:lane + units] = part[cut].astype(BF16)
                rs_out[s, place, :, lane + units:lane + half] = jnp.broadcast_to(
                    extra[cut], (piece, half - units)).astype(BF16)

    def scatter(s):
        def ring(src, o, to):
            return pltpu.make_async_remote_copy(
                src_ref=src, dst_ref=rs_in.at[s, o], send_sem=rs_send.at[s, o], recv_sem=rs_recv.at[s, o],
                device_id={"ra": at(to)}, device_id_type=MESH)

        copies = {o: ring(rs_out.at[s, at(o)], o, o) for o in near if o not in (hop, n_ra - hop)}
        copies |= {o: ring(rs_out.at[s, at(o)], o, o - hop) for o in ahead}
        copies |= {o: ring(rs_out.at[s, at(o)], o, o + hop) for o in behind}
        copies |= {o: ring(sums.at[s, i], o, o) for i, o in enumerate((n_ra - hop, hop))}
        return copies

    def via(o):
        return o - hop if o in ahead else o + hop if o in behind else o

    def ag_copy(s, o, slot):
        return pltpu.make_async_remote_copy(
            src_ref=ag_out.at[s], dst_ref=ag_in.at[s, slot], send_sem=ag_send.at[s, o],
            recv_sem=ag_recv.at[s, o], device_id={"ra": at(o)}, device_id_type=MESH)

    def ar_copy(s, g, o, slot):
        return pltpu.make_async_remote_copy(
            src_ref=ar_in.at[s, g, cb], dst_ref=ar_in.at[s, g, slot], send_sem=ar_send.at[s, g, o],
            recv_sem=ar_recv.at[s, g, o], device_id={"cb": lax.rem(cb + o, n_cb)}, device_id_type=MESH)

    rs = [scatter(s) for s in range(2)]
    relays = (n_ra - hop, hop)
    free = [o for o in far_first(n_ra) if o not in relays]

    with scope("load"):
        for c in loads[:4]:
            c.wait()
    with scope("project_first"):
        xf = x_v[...].astype(F32)
        for i in range(n_ra):
            x_f[i] = xf[i * piece:(i + 1) * piece]
        project(0, xf, range(n_ra))
    with scope("send_first"):
        for o in free:
            pl.when(turn + via(o) >= n_ra)(rs[0][o].start)
    with scope("send_ready"):
        for p in near:
            @pl.when(turn + p < n_ra)
            def _():
                pl.semaphore_wait(ready.at[p], 1)
                for o in free:
                    if via(o) == p:
                        rs[0][o].start()

    @pl.when(turn == 0)
    def _():
        pl.semaphore_wait(column, n_ra - 1)
        for o in range(1, n_cb):
            pl.semaphore_signal(row, 1, device_id={"cb": lax.rem(cb + o, n_cb)}, device_id_type=MESH)
        pl.semaphore_wait(row, n_cb - 1)
        for o in far_first(n_ra):
            pl.semaphore_signal(all_in, 1, device_id={"ra": at(o)}, device_id_type=MESH)

    for s in range(2):
        for i, (o, far) in enumerate(zip(relays, (behind, ahead))):
            part = rs_out[s, at(o)].astype(F32)
            for f in far:
                with scope(f"relay_wait{s}_{f}"):
                    rs[s][f].wait_recv()
                part = part + rs_in[s, f].astype(F32)
            sums[s, i] = part.astype(BF16)
            rs[s][o].start()
        total = rs_out[s, ra].astype(F32)
        for o in sorted(near, key=lambda o: min(o, n_ra - o)):
            with scope(f"scatter_wait{s}_{o}"):
                rs[s][o].wait_recv()
            total = total + rs_in[s, o].astype(F32)
        sumsq = total[:, units:units + 1] + total[:, half + units:half + units + 1]
        scale = lax.rsqrt(sumsq / width + 1e-06)
        g = total[:, :units] * scale
        hidden = (g / (1.0 + jnp.exp(-g)) * (total[:, half:half + units] * scale)).astype(BF16)
        ag_out[s] = hidden
        ag_in[s, ra] = hidden
        ag = [ag_copy(s, o, ra) for o in far_first(n_ra)]
        for c in ag:
            c.start()
        loads[4 * s + 4].wait()
        for c in rs[s].values():
            c.wait_send()
        if s == 0:
            for c in loads[5:8]:
                c.wait()

        ar = []

        def down(g):
            for o in groups[g]:
                if o:
                    with scope(f"gather_wait{s}_{o}"):
                        ag_copy(s, n_ra - o, at(o)).wait_recv()
            h = jnp.concatenate([ag_in[s, at(o)].astype(F32) for o in groups[g]], axis=0).astype(BF16)
            ar_in[s, g, cb] = jnp.dot(h, down_v[s], preferred_element_type=F32).astype(BF16)
            for o in far_first(n_cb):
                c = ar_copy(s, g, o, cb)
                c.start()
                ar.append(c)

        def finish(g):
            with scope(f"cb_wait{s}_{g}"):
                for o in far_first(n_cb):
                    ar_copy(s, g, o, lax.rem(cb + n_cb - o, n_cb)).wait_recv()
            branch = ar_in[s, g, 0].astype(F32)
            for c in range(1, n_cb):
                branch = branch + ar_in[s, g, c].astype(F32)
            places = [at(o) for o in groups[g]]
            old = jnp.concatenate([x_f[p] for p in places], axis=0)
            result = (0.5 * old + 0.5 * branch).astype(BF16)
            if s == 1:
                for i, p in enumerate(places):
                    out[p] = result[i * piece:(i + 1) * piece]
                return
            new = result.astype(F32)
            for i, p in enumerate(places):
                x_f[p] = new[i * piece:(i + 1) * piece]
            project(1, new, places)
            for o in groups[g]:
                if o in free:
                    rs[1][o].start()

        if s == 0:
            with scope("all_in"):
                @pl.when(turn > 0)
                def _():
                    pl.semaphore_wait(all_in, 1)
        for g in range(GROUPS):
            down(g)
        for c in ag:
            c.wait_send()
        for g in range(GROUPS):
            finish(g)
        for c in ar:
            c.wait_send()


def per_device(tokens, first_gain, first_gate, first_up, first_down,
               second_gain, second_gate, second_up, second_down):
    n_ra, n_cb = lax.axis_size("ra"), lax.axis_size("cb")
    rows, cols = tokens.shape
    units = first_gate.shape[1]
    half = (units // LANES + 1) * LANES
    piece = rows // n_ra
    dma = pltpu.SemaphoreType.DMA
    any_spec = pl.BlockSpec(memory_space=pl.ANY)
    out = pl.pallas_call(
        functools.partial(fused, n_ra, n_cb),
        out_shape=jax.ShapeDtypeStruct((n_ra, piece, cols), BF16),
        in_specs=[any_spec] * 9,
        out_specs=pl.BlockSpec(memory_space=pltpu.VMEM),
        scratch_shapes=[
            pltpu.VMEM((rows, cols), BF16),
            pltpu.VMEM((2, 1, cols), BF16),
            pltpu.VMEM((2, units, cols), BF16),
            pltpu.VMEM((2, units, cols), BF16),
            pltpu.VMEM((2, units, cols), BF16),
            pltpu.VMEM((n_ra, piece, cols), F32),
            pltpu.VMEM((2, n_ra, piece, 2 * half), BF16),
            pltpu.VMEM((2, 2, piece, 2 * half), BF16),
            pltpu.VMEM((2, n_ra, piece, 2 * half), BF16),
            pltpu.VMEM((2, piece, units), BF16),
            pltpu.VMEM((2, n_ra, piece, units), BF16),
            pltpu.VMEM((2, GROUPS, n_cb, rows // GROUPS, cols), BF16),
            pltpu.SemaphoreType.REGULAR((n_ra,)),
            pltpu.SemaphoreType.REGULAR,
            pltpu.SemaphoreType.REGULAR,
            pltpu.SemaphoreType.REGULAR,
            dma((9,)),
            dma((2, n_ra)), dma((2, n_ra)),
            dma((2, n_ra)), dma((2, n_ra)),
            dma((2, GROUPS, n_cb)), dma((2, GROUPS, n_cb)),
        ],
        compiler_params=pltpu.CompilerParams(collective_id=0, has_side_effects=True),
    )(tokens, first_gain.reshape(1, -1), first_gate.T, first_up.T, first_down,
      second_gain.reshape(1, -1), second_gate.T, second_up.T, second_down)
    return out.reshape(rows, cols)


def solution(mesh):
    placed = (
        P("grp", "ra"),
        P("ra"), P("ra", "cb"), P("ra", "cb"), P("cb", "ra"),
        P("ra"), P("ra", "cb"), P("ra", "cb"), P("cb", "ra"),
    )
    return jax.shard_map(
        per_device, mesh=mesh, in_specs=placed, out_specs=P("grp", "ra"), check_vma=False
    )
```

```python
import functools

import jax
import jax.numpy as jnp
from jax import lax
from jax.experimental import pallas as pl
from jax.experimental.pallas import tpu as pltpu
from jax.sharding import PartitionSpec as P

MESH = pl.DeviceIdType.MESH
LANES = 128
BF16 = jnp.bfloat16
F32 = jnp.float32
scope = jax.named_scope
GROUPS = (4, 4)


def far_first(n):
    return sorted(range(1, n), key=lambda o: -min(o, n - o))


def groups_of(n):
    order = far_first(n) + [0]
    return [[order[i:i + n // k] for i in range(0, n, n // k)] for k in GROUPS]


def fused(n_ra, n_cb, tokens, gain1, gate1, up1, down1, gain2, gate2, up2, down2, out,
          x_v, gain_v, gate_v, up_v, down_v, x_f,
          rs_out, sums, rs_in, ag_out, ag_in, ar_in1, ar_in2,
          ready, column, row, all_in, load_sem, rs_send, rs_recv, ag_send, ag_recv, ar_send, ar_recv):
    ra = lax.axis_index("ra")
    cb = lax.axis_index("cb")
    rows, cols = x_v.shape
    piece = rows // n_ra
    units = gate_v.shape[1]
    half = rs_in.shape[3] // 2
    width = cols * n_ra
    ar_ins = (ar_in1, ar_in2)
    all_groups = groups_of(n_ra)

    hop = n_ra // 4
    ahead = list(range(hop + 1, n_ra // 2 + 1))
    behind = list(range(n_ra // 2 + 1, n_ra - hop))
    near = list(range(1, hop + 1)) + list(range(n_ra - hop, n_ra))

    relays = (n_ra - hop, hop)

    def at(o):
        return lax.rem(ra + o, n_ra)

    loads = [pltpu.make_async_copy(tokens, x_v, load_sem.at[0])]
    for s, (gn, gt, up, dn) in enumerate(((gain1, gate1, up1, down1), (gain2, gate2, up2, down2))):
        loads += [
            pltpu.make_async_copy(gn, gain_v.at[s], load_sem.at[4 * s + 1]),
            pltpu.make_async_copy(gt, gate_v.at[s], load_sem.at[4 * s + 2]),
            pltpu.make_async_copy(up, up_v.at[s], load_sem.at[4 * s + 3]),
            pltpu.make_async_copy(dn, down_v.at[s], load_sem.at[4 * s + 4]),
        ]
    for c in loads:
        c.start()

    turn = lax.rem(ra + n_ra - 1, n_ra)
    odd = lax.rem(cb, 2) == 1
    partner = {"cb": cb + 1 - 2 * lax.rem(cb, 2)}

    def later(o):
        return turn + o < n_ra

    barrier = pltpu.get_barrier_semaphore()

    @pl.when(turn == 0)
    def _():
        for o in range(1, n_cb):
            pl.semaphore_signal(barrier, 1, device_id={"cb": lax.rem(cb + o, n_cb)}, device_id_type=MESH)

    @pl.when(jnp.logical_and(turn > 0, jnp.logical_not(odd)))
    def _():
        pl.semaphore_signal(barrier, 1, device_id=partner, device_id_type=MESH)

    with scope("barrier"):
        pl.semaphore_wait(barrier, jnp.where(turn == 0, n_cb - 1, jnp.where(odd, 2, 1)))

    @pl.when(jnp.logical_and(turn < n_ra - 1, odd))
    def _():
        pl.semaphore_signal(barrier, 1, device_id={"ra": lax.rem(ra + 1, n_ra)}, device_id_type=MESH)

    @pl.when(jnp.logical_and(turn > 0, odd))
    def _():
        pl.semaphore_signal(barrier, 1, device_id=partner, device_id_type=MESH)

    for o in near:
        @pl.when(turn >= o)
        def _():
            pl.semaphore_signal(ready.at[near.index(o)], 1, device_id={"ra": at(n_ra - o)}, device_id_type=MESH)

    @pl.when(turn > 0)
    def _():
        pl.semaphore_signal(column, 1, device_id={"ra": lax.rem(ra + n_ra - turn, n_ra)}, device_id_type=MESH)

    def project(s, xf, places):
        sq = jnp.sum(xf * xf, axis=1, keepdims=True)
        hi = sq.astype(BF16).astype(F32)
        normed = (xf * gain_v[s].astype(F32)).astype(BF16)
        for w, lane, extra in ((gate_v, 0, hi), (up_v, half, sq - hi)):
            part = lax.dot_general(normed, w[s], (((1,), (1,)), ((), ())), preferred_element_type=F32)
            for i, place in enumerate(places):
                cut = slice(i * piece, (i + 1) * piece)
                rs_out[s, place, :, lane:lane + units] = part[cut].astype(BF16)
                rs_out[s, place, :, lane + units:lane + half] = jnp.broadcast_to(
                    extra[cut], (piece, half - units)).astype(BF16)

    def batch(o):
        return 0 if o in ahead else 1 if o in behind else 2 if o == hop else 3 if o == n_ra - hop else 4

    def all_of(ref, send_sem, recv_sem):
        return pltpu.make_async_remote_copy(
            src_ref=ref, dst_ref=ref, send_sem=send_sem, recv_sem=recv_sem,
            device_id={"ra": at(1)}, device_id_type=MESH)

    def scattered(s, count, which=0):
        return all_of(rs_in.at[s, pl.ds(0, count)], rs_send.at[s], rs_recv.at[s, which])

    def scatter(s):
        def ring(src, o, to):
            return pltpu.make_async_remote_copy(
                src_ref=src, dst_ref=rs_in.at[s, o], send_sem=rs_send.at[s], recv_sem=rs_recv.at[s, batch(o)],
                device_id={"ra": at(to)}, device_id_type=MESH)

        copies = {o: ring(rs_out.at[s, at(o)], o, o) for o in near if o not in (hop, n_ra - hop)}
        copies |= {o: ring(rs_out.at[s, at(o)], o, o - hop) for o in ahead}
        copies |= {o: ring(rs_out.at[s, at(o)], o, o + hop) for o in behind}
        copies |= {o: ring(sums.at[s, i], o, o) for i, o in enumerate((n_ra - hop, hop))}
        return copies

    def via(o):
        return o - hop if o in ahead else o + hop if o in behind else o

    def ag_copy(s, o):
        seen = n_ra - o
        group = [seen in g for g in all_groups[s]].index(True)
        return pltpu.make_async_remote_copy(
            src_ref=ag_out.at[s], dst_ref=ag_in.at[s, ra], send_sem=ag_send.at[s],
            recv_sem=ag_recv.at[s, group], device_id={"ra": at(o)}, device_id_type=MESH)

    def gathered(s, count, recv_sem):
        return all_of(ag_in.at[s, pl.ds(0, count)], ag_send.at[s], recv_sem)

    def summed(s, g):
        return all_of(ar_ins[s].at[g, pl.ds(0, n_cb - 1)], ar_send.at[s, g], ar_recv.at[s, g])

    rs = [scatter(s) for s in range(2)]
    free = [o for o in far_first(n_ra) if o not in relays]

    with scope("load"):
        for c in loads[:4]:
            c.wait()
    with scope("project_first"):
        xf = x_v[...].astype(F32)
        for i in range(n_ra):
            x_f[i] = xf[i * piece:(i + 1) * piece]
        project(0, xf, range(n_ra))
    with scope("send_first"):
        for o in free:
            pl.when(jnp.logical_not(later(via(o))))(rs[0][o].start)
    with scope("send_ready"):
        for p in near:
            @pl.when(later(p))
            def _():
                pl.semaphore_wait(ready.at[near.index(p)], 1)
                for o in free:
                    if via(o) == p:
                        rs[0][o].start()

    @pl.when(turn == 0)
    def _():
        pl.semaphore_wait(column, n_ra - 1)
        for o in range(1, n_cb):
            pl.semaphore_signal(row, 1, device_id={"cb": lax.rem(cb + o, n_cb)}, device_id_type=MESH)
        pl.semaphore_wait(row, n_cb - 1)
        for o in far_first(n_ra):
            pl.semaphore_signal(all_in, 1, device_id={"ra": at(o)}, device_id_type=MESH)

    for s in range(2):
        for i, (o, far) in enumerate(zip(relays, (behind, ahead))):
            part = rs_out[s, at(o)].astype(F32)
            with scope(f"relay_wait{s}_{o}"):
                scattered(s, len(far), batch(far[0])).wait_recv()
            for f in far:
                part = part + rs_in[s, f].astype(F32)
            sums[s, i] = part.astype(BF16)
            rs[s][o].start()
        total = rs_out[s, ra].astype(F32)
        direct = [o for o in near if o not in relays]
        with scope(f"scatter_wait{s}_direct"):
            scattered(s, len(direct), batch(direct[0])).wait_recv()
        for o in direct:
            total = total + rs_in[s, o].astype(F32)
        for o in relays:
            with scope(f"scatter_wait{s}_{o}"):
                scattered(s, 1, batch(o)).wait_recv()
            total = total + rs_in[s, o].astype(F32)
        sumsq = total[:, units:units + 1] + total[:, half + units:half + units + 1]
        scale = lax.rsqrt(sumsq / width + 1e-06)
        g = total[:, :units] * scale
        hidden = (g / (1.0 + jnp.exp(-g)) * (total[:, half:half + units] * scale)).astype(BF16)
        ag_out[s] = hidden
        ag_in[s, ra] = hidden
        ag = [ag_copy(s, o) for o in far_first(n_ra)]
        if s == 1:
            for early in (True, False):
                for o, c in zip(far_first(n_ra), ag):
                    pl.when((at(o) < n_ra // 2) == early)(c.start)
        else:
            for c in ag:
                c.start()
        loads[4 * s + 4].wait()
        scattered(s, n_ra - 1).wait_send()
        if s == 0:
            for c in loads[5:8]:
                c.wait()

        groups = all_groups[s]
        ar_in = ar_ins[s]

        def down(g):
            with scope(f"gather_wait{s}_{g}"):
                count = sum(o != 0 for o in groups[g])
                gathered(s, count, ag_recv.at[s, g]).wait_recv()
            h = jnp.concatenate([ag_in[s, at(o)].astype(F32) for o in groups[g]], axis=0).astype(BF16)
            ar_in[g, cb] = jnp.dot(h, down_v[s], preferred_element_type=F32).astype(BF16)
            for o in far_first(n_cb):
                pltpu.make_async_remote_copy(
                    src_ref=ar_in.at[g, cb], dst_ref=ar_in.at[g, cb], send_sem=ar_send.at[s, g],
                    recv_sem=ar_recv.at[s, g], device_id={"cb": lax.rem(cb + o, n_cb)}, device_id_type=MESH).start()

        def finish(g):
            with scope(f"cb_wait{s}_{g}"):
                summed(s, g).wait_recv()
            branch = ar_in[g, 0].astype(F32)
            for c in range(1, n_cb):
                branch = branch + ar_in[g, c].astype(F32)
            places = [at(o) for o in groups[g]]
            old = jnp.concatenate([x_f[p] for p in places], axis=0)
            result = (0.5 * old + 0.5 * branch).astype(BF16)
            if s == 1:
                for i, p in enumerate(places):
                    out[p] = result[i * piece:(i + 1) * piece]
                return
            new = result.astype(F32)
            for i, p in enumerate(places):
                x_f[p] = new[i * piece:(i + 1) * piece]
            project(1, new, places)
            for o in groups[g]:
                if o in free:
                    rs[1][o].start()

        if s == 0:
            with scope("all_in"):
                @pl.when(turn > 0)
                def _():
                    pl.semaphore_wait(all_in, 1)
        for g in range(len(groups)):
            down(g)
        gathered(s, n_ra - 1, ag_recv.at[s, 0]).wait_send()
        for g in range(len(groups)):
            finish(g)
        for g in range(len(groups)):
            summed(s, g).wait_send()


def per_device(tokens, first_gain, first_gate, first_up, first_down,
               second_gain, second_gate, second_up, second_down):
    n_ra, n_cb = lax.axis_size("ra"), lax.axis_size("cb")
    rows, cols = tokens.shape
    units = first_gate.shape[1]
    half = (units // LANES + 1) * LANES
    piece = rows // n_ra
    dma = pltpu.SemaphoreType.DMA
    any_spec = pl.BlockSpec(memory_space=pl.ANY)
    out = pl.pallas_call(
        functools.partial(fused, n_ra, n_cb),
        out_shape=pltpu.VMEM((n_ra, piece, cols), BF16),
        in_specs=[any_spec] * 9,
        out_specs=pl.BlockSpec(memory_space=pltpu.VMEM),
        scratch_shapes=[
            pltpu.VMEM((rows, cols), BF16),
            pltpu.VMEM((2, 1, cols), BF16),
            pltpu.VMEM((2, units, cols), BF16),
            pltpu.VMEM((2, units, cols), BF16),
            pltpu.VMEM((2, units, cols), BF16),
            pltpu.VMEM((n_ra, piece, cols), F32),
            pltpu.VMEM((2, n_ra, piece, 2 * half), BF16),
            pltpu.VMEM((2, 2, piece, 2 * half), BF16),
            pltpu.VMEM((2, n_ra, piece, 2 * half), BF16),
            pltpu.VMEM((2, piece, units), BF16),
            pltpu.VMEM((2, n_ra, piece, units), BF16),
            *(pltpu.VMEM((k, n_cb, rows // k, cols), BF16) for k in GROUPS),
            pltpu.SemaphoreType.REGULAR((n_ra // 2,)),
            pltpu.SemaphoreType.REGULAR,
            pltpu.SemaphoreType.REGULAR,
            pltpu.SemaphoreType.REGULAR,
            dma((9,)),
            dma((2,)), dma((2, 5)),
            dma((2,)), dma((2, max(GROUPS))),
            dma((2, max(GROUPS))), dma((2, max(GROUPS))),
        ],
        compiler_params=pltpu.CompilerParams(collective_id=0, has_side_effects=True),
    )(tokens, first_gain.reshape(1, -1), first_gate.T, first_up.T, first_down,
      second_gain.reshape(1, -1), second_gate.T, second_up.T, second_down)
    return out.reshape(rows, cols)


def solution(mesh):
    placed = (
        P("grp", "ra"),
        P("ra"), P("ra", "cb"), P("ra", "cb"), P("cb", "ra"),
        P("ra"), P("ra", "cb"), P("ra", "cb"), P("cb", "ra"),
    )
    return jax.shard_map(
        per_device, mesh=mesh, in_specs=placed, out_specs=P("grp", "ra"), check_vma=False
    )
```

```python
import functools

import jax
import jax.numpy as jnp
from jax import lax
from jax.experimental import pallas as pl
from jax.experimental.pallas import tpu as pltpu
from jax.sharding import PartitionSpec as P

MESH = pl.DeviceIdType.MESH
LANES = 128
BF16 = jnp.bfloat16
F32 = jnp.float32
scope = jax.named_scope
GROUPS = (8, 4)


def far_first(n):
    return sorted(range(1, n), key=lambda o: -min(o, n - o))


def groups_of(n):
    order = far_first(n) + [0]
    return [[order[i:i + n // k] for i in range(0, n, n // k)] for k in GROUPS]


def fused(n_ra, n_cb, tokens, gain1, gate1, up1, down1, gain2, gate2, up2, down2, out,
          x_v, gain_v, gate_v, up_v, down_v, x_f,
          rs_out, sums, rs_in, ag_out, ag_in, ar_in1, ar_in2,
          ready, column, row, all_in, load_sem, rs_send, rs_recv, ag_send, ag_recv, ar_send, ar_recv):
    ra = lax.axis_index("ra")
    cb = lax.axis_index("cb")
    rows, cols = x_v.shape
    piece = rows // n_ra
    units = gate_v.shape[1]
    half = rs_in.shape[3] // 2
    width = cols * n_ra
    ar_ins = (ar_in1, ar_in2)
    all_groups = groups_of(n_ra)

    hop = n_ra // 4
    ahead = list(range(hop + 1, n_ra // 2 + 1))
    behind = list(range(n_ra // 2 + 1, n_ra - hop))
    near = list(range(1, hop + 1)) + list(range(n_ra - hop, n_ra))

    relays = (n_ra - hop, hop)

    def at(o):
        return lax.rem(ra + o, n_ra)

    loads = [pltpu.make_async_copy(tokens, x_v, load_sem.at[0])]
    for s, (gn, gt, up, dn) in enumerate(((gain1, gate1, up1, down1), (gain2, gate2, up2, down2))):
        loads += [
            pltpu.make_async_copy(gn, gain_v.at[s], load_sem.at[4 * s + 1]),
            pltpu.make_async_copy(gt, gate_v.at[s], load_sem.at[4 * s + 2]),
            pltpu.make_async_copy(up, up_v.at[s], load_sem.at[4 * s + 3]),
            pltpu.make_async_copy(dn, down_v.at[s], load_sem.at[4 * s + 4]),
        ]
    for c in loads:
        c.start()

    turn = lax.rem(ra + n_ra - 1, n_ra)
    odd = lax.rem(cb, 2) == 1
    partner = {"cb": cb + 1 - 2 * lax.rem(cb, 2)}

    def later(o):
        return turn + o < n_ra

    barrier = pltpu.get_barrier_semaphore()

    @pl.when(turn == 0)
    def _():
        for o in range(1, n_cb):
            pl.semaphore_signal(barrier, 1, device_id={"cb": lax.rem(cb + o, n_cb)}, device_id_type=MESH)

    @pl.when(jnp.logical_and(turn > 0, jnp.logical_not(odd)))
    def _():
        pl.semaphore_signal(barrier, 1, device_id=partner, device_id_type=MESH)

    with scope("barrier"):
        pl.semaphore_wait(barrier, jnp.where(turn == 0, n_cb - 1, jnp.where(odd, 2, 1)))

    @pl.when(jnp.logical_and(turn < n_ra - 1, odd))
    def _():
        pl.semaphore_signal(barrier, 1, device_id={"ra": lax.rem(ra + 1, n_ra)}, device_id_type=MESH)

    @pl.when(jnp.logical_and(turn > 0, odd))
    def _():
        pl.semaphore_signal(barrier, 1, device_id=partner, device_id_type=MESH)

    for o in near:
        @pl.when(turn >= o)
        def _():
            pl.semaphore_signal(ready.at[near.index(o)], 1, device_id={"ra": at(n_ra - o)}, device_id_type=MESH)

    @pl.when(turn > 0)
    def _():
        pl.semaphore_signal(column, 1, device_id={"ra": lax.rem(ra + n_ra - turn, n_ra)}, device_id_type=MESH)

    def project(s, xf, places):
        sq = jnp.sum(xf * xf, axis=1, keepdims=True)
        hi = sq.astype(BF16).astype(F32)
        normed = (xf * gain_v[s].astype(F32)).astype(BF16)
        for w, lane, extra in ((gate_v, 0, hi), (up_v, half, sq - hi)):
            part = lax.dot_general(normed, w[s], (((1,), (1,)), ((), ())), preferred_element_type=F32)
            for i, place in enumerate(places):
                cut = slice(i * piece, (i + 1) * piece)
                rs_out[s, place, :, lane:lane + units] = part[cut].astype(BF16)
                rs_out[s, place, :, lane + units:lane + half] = jnp.broadcast_to(
                    extra[cut], (piece, half - units)).astype(BF16)

    def batch(o):
        return 0 if o in ahead else 1 if o in behind else 2 if o == hop else 3 if o == n_ra - hop else 4

    def all_of(ref, send_sem, recv_sem):
        return pltpu.make_async_remote_copy(
            src_ref=ref, dst_ref=ref, send_sem=send_sem, recv_sem=recv_sem,
            device_id={"ra": at(1)}, device_id_type=MESH)

    def scattered(s, count, which=0):
        return all_of(rs_in.at[s, pl.ds(0, count)], rs_send.at[s], rs_recv.at[s, which])

    def scatter(s):
        def ring(src, o, to):
            return pltpu.make_async_remote_copy(
                src_ref=src, dst_ref=rs_in.at[s, o], send_sem=rs_send.at[s], recv_sem=rs_recv.at[s, batch(o)],
                device_id={"ra": at(to)}, device_id_type=MESH)

        copies = {o: ring(rs_out.at[s, at(o)], o, o) for o in near if o not in (hop, n_ra - hop)}
        copies |= {o: ring(rs_out.at[s, at(o)], o, o - hop) for o in ahead}
        copies |= {o: ring(rs_out.at[s, at(o)], o, o + hop) for o in behind}
        copies |= {o: ring(sums.at[s, i], o, o) for i, o in enumerate((n_ra - hop, hop))}
        return copies

    def via(o):
        return o - hop if o in ahead else o + hop if o in behind else o

    def ag_copy(s, o):
        seen = n_ra - o
        group = [seen in g for g in all_groups[s]].index(True)
        return pltpu.make_async_remote_copy(
            src_ref=ag_out.at[s], dst_ref=ag_in.at[s, ra], send_sem=ag_send.at[s],
            recv_sem=ag_recv.at[s, group], device_id={"ra": at(o)}, device_id_type=MESH)

    def gathered(s, count, recv_sem):
        return all_of(ag_in.at[s, pl.ds(0, count)], ag_send.at[s], recv_sem)

    def summed(s, g):
        return all_of(ar_ins[s].at[g, pl.ds(0, n_cb - 1)], ar_send.at[s, g], ar_recv.at[s, g])

    rs = [scatter(s) for s in range(2)]
    free = [o for o in far_first(n_ra) if o not in relays]

    with scope("load"):
        for c in loads[:4]:
            c.wait()
    with scope("project_first"):
        xf = x_v[...].astype(F32)
        for i in range(n_ra):
            x_f[i] = xf[i * piece:(i + 1) * piece]
        project(0, xf, range(n_ra))
    with scope("send_first"):
        for o in free:
            pl.when(jnp.logical_not(later(via(o))))(rs[0][o].start)
    with scope("send_ready"):
        for p in near:
            @pl.when(later(p))
            def _():
                pl.semaphore_wait(ready.at[near.index(p)], 1)
                for o in free:
                    if via(o) == p:
                        rs[0][o].start()

    @pl.when(turn == 0)
    def _():
        pl.semaphore_wait(column, n_ra - 1)
        for o in range(1, n_cb):
            pl.semaphore_signal(row, 1, device_id={"cb": lax.rem(cb + o, n_cb)}, device_id_type=MESH)
        pl.semaphore_wait(row, n_cb - 1)
        for o in far_first(n_ra):
            pl.semaphore_signal(all_in, 1, device_id={"ra": at(o)}, device_id_type=MESH)

    for s in range(2):
        for i, (o, far) in enumerate(zip(relays, (behind, ahead))):
            part = rs_out[s, at(o)].astype(F32)
            with scope(f"relay_wait{s}_{o}"):
                scattered(s, len(far), batch(far[0])).wait_recv()
            for f in far:
                part = part + rs_in[s, f].astype(F32)
            sums[s, i] = part.astype(BF16)
            rs[s][o].start()
        total = rs_out[s, ra].astype(F32)
        direct = [o for o in near if o not in relays]
        with scope(f"scatter_wait{s}_direct"):
            scattered(s, len(direct), batch(direct[0])).wait_recv()
        for o in direct:
            total = total + rs_in[s, o].astype(F32)
        for o in relays:
            with scope(f"scatter_wait{s}_{o}"):
                scattered(s, 1, batch(o)).wait_recv()
            total = total + rs_in[s, o].astype(F32)
        sumsq = total[:, units:units + 1] + total[:, half + units:half + units + 1]
        scale = lax.rsqrt(sumsq / width + 1e-06)
        g = total[:, :units] * scale
        hidden = (g / (1.0 + jnp.exp(-g)) * (total[:, half:half + units] * scale)).astype(BF16)
        ag_out[s] = hidden
        ag_in[s, ra] = hidden
        ag = [ag_copy(s, o) for o in far_first(n_ra)]
        if s == 1:
            for early in (True, False):
                for o, c in zip(far_first(n_ra), ag):
                    pl.when((at(o) < n_ra // 2) == early)(c.start)
        else:
            for c in ag:
                c.start()
        loads[4 * s + 4].wait()
        scattered(s, n_ra - 1).wait_send()
        if s == 0:
            for c in loads[5:8]:
                c.wait()

        groups = all_groups[s]
        ar_in = ar_ins[s]

        def down(g):
            with scope(f"gather_wait{s}_{g}"):
                count = sum(o != 0 for o in groups[g])
                gathered(s, count, ag_recv.at[s, g]).wait_recv()
            h = jnp.concatenate([ag_in[s, at(o)].astype(F32) for o in groups[g]], axis=0).astype(BF16)
            ar_in[g, cb] = jnp.dot(h, down_v[s], preferred_element_type=F32).astype(BF16)
            for o in far_first(n_cb):
                pltpu.make_async_remote_copy(
                    src_ref=ar_in.at[g, cb], dst_ref=ar_in.at[g, cb], send_sem=ar_send.at[s, g],
                    recv_sem=ar_recv.at[s, g], device_id={"cb": lax.rem(cb + o, n_cb)}, device_id_type=MESH).start()

        def finish(g):
            with scope(f"cb_wait{s}_{g}"):
                summed(s, g).wait_recv()
            branch = ar_in[g, 0].astype(F32)
            for c in range(1, n_cb):
                branch = branch + ar_in[g, c].astype(F32)
            places = [at(o) for o in groups[g]]
            old = jnp.concatenate([x_f[p] for p in places], axis=0)
            result = (0.5 * old + 0.5 * branch).astype(BF16)
            if s == 1:
                for i, p in enumerate(places):
                    out[p] = result[i * piece:(i + 1) * piece]
                return
            new = result.astype(F32)
            for i, p in enumerate(places):
                x_f[p] = new[i * piece:(i + 1) * piece]
            project(1, new, places)
            for o in groups[g]:
                if o in free:
                    rs[1][o].start()

        if s == 0:
            with scope("all_in"):
                @pl.when(turn > 0)
                def _():
                    pl.semaphore_wait(all_in, 1)
        for g in range(len(groups)):
            down(g)
        gathered(s, n_ra - 1, ag_recv.at[s, 0]).wait_send()
        for g in range(len(groups)):
            finish(g)
        for g in range(len(groups)):
            summed(s, g).wait_send()


def per_device(tokens, first_gain, first_gate, first_up, first_down,
               second_gain, second_gate, second_up, second_down):
    n_ra, n_cb = lax.axis_size("ra"), lax.axis_size("cb")
    rows, cols = tokens.shape
    units = first_gate.shape[1]
    half = (units // LANES + 1) * LANES
    piece = rows // n_ra
    dma = pltpu.SemaphoreType.DMA
    any_spec = pl.BlockSpec(memory_space=pl.ANY)
    out = pl.pallas_call(
        functools.partial(fused, n_ra, n_cb),
        out_shape=pltpu.VMEM((n_ra, piece, cols), BF16),
        in_specs=[any_spec] * 9,
        out_specs=pl.BlockSpec(memory_space=pltpu.VMEM),
        scratch_shapes=[
            pltpu.VMEM((rows, cols), BF16),
            pltpu.VMEM((2, 1, cols), BF16),
            pltpu.VMEM((2, units, cols), BF16),
            pltpu.VMEM((2, units, cols), BF16),
            pltpu.VMEM((2, units, cols), BF16),
            pltpu.VMEM((n_ra, piece, cols), F32),
            pltpu.VMEM((2, n_ra, piece, 2 * half), BF16),
            pltpu.VMEM((2, 2, piece, 2 * half), BF16),
            pltpu.VMEM((2, n_ra, piece, 2 * half), BF16),
            pltpu.VMEM((2, piece, units), BF16),
            pltpu.VMEM((2, n_ra, piece, units), BF16),
            *(pltpu.VMEM((k, n_cb, rows // k, cols), BF16) for k in GROUPS),
            pltpu.SemaphoreType.REGULAR((n_ra // 2,)),
            pltpu.SemaphoreType.REGULAR,
            pltpu.SemaphoreType.REGULAR,
            pltpu.SemaphoreType.REGULAR,
            dma((9,)),
            dma((2,)), dma((2, 5)),
            dma((2,)), dma((2, max(GROUPS))),
            dma((2, max(GROUPS))), dma((2, max(GROUPS))),
        ],
        compiler_params=pltpu.CompilerParams(collective_id=0, has_side_effects=True),
    )(tokens, first_gain.reshape(1, -1), first_gate.T, first_up.T, first_down,
      second_gain.reshape(1, -1), second_gate.T, second_up.T, second_down)
    return out.reshape(rows, cols)


def solution(mesh):
    placed = (
        P("grp", "ra"),
        P("ra"), P("ra", "cb"), P("ra", "cb"), P("cb", "ra"),
        P("ra"), P("ra", "cb"), P("ra", "cb"), P("cb", "ra"),
    )
    return jax.shard_map(
        per_device, mesh=mesh, in_specs=placed, out_specs=P("grp", "ra"), check_vma=False
    )
```

```python
import functools

import jax
import jax.numpy as jnp
from jax import lax
from jax.experimental import pallas as pl
from jax.experimental.pallas import tpu as pltpu
from jax.sharding import PartitionSpec as P

MESH = pl.DeviceIdType.MESH
LANES = 128
BF16 = jnp.bfloat16
F32 = jnp.float32
scope = jax.named_scope
GROUPS = (8, 4)


def far_first(n):
    return sorted(range(1, n), key=lambda o: -min(o, n - o))


def groups_of(n):
    order = far_first(n) + [0]
    return [[order[i:i + n // k] for i in range(0, n, n // k)] for k in GROUPS]


def fused(n_ra, n_cb, tokens, gain1, gate1, up1, down1, gain2, gate2, up2, down2, out,
          x_v, gain_v, gate_v, up_v, down_v, x_f,
          rs_out, sums, rs_in, sq_out, sq_sums, sq_in, ag_out, ag_in, ar_in1, ar_in2,
          ready, column, row, all_in, load_sem, rs_send, rs_recv, sq_send, sq_recv, ag_send, ag_recv, ar_send, ar_recv):
    ra = lax.axis_index("ra")
    cb = lax.axis_index("cb")
    rows, cols = x_v.shape
    piece = rows // n_ra
    units = gate_v.shape[1]
    main = units // LANES * LANES
    rest = units - main
    diagonal = lax.broadcasted_iota(jnp.int32, (piece, LANES), 0) == lax.broadcasted_iota(jnp.int32, (piece, LANES), 1)
    width = cols * n_ra
    ar_ins = (ar_in1, ar_in2)
    all_groups = groups_of(n_ra)

    hop = n_ra // 4
    ahead = list(range(hop + 1, n_ra // 2 + 1))
    behind = list(range(n_ra // 2 + 1, n_ra - hop))
    near = list(range(1, hop + 1)) + list(range(n_ra - hop, n_ra))

    relays = (n_ra - hop, hop)

    def at(o):
        return lax.rem(ra + o, n_ra)

    loads = [pltpu.make_async_copy(tokens, x_v, load_sem.at[0])]
    for s, (gn, gt, up, dn) in enumerate(((gain1, gate1, up1, down1), (gain2, gate2, up2, down2))):
        loads += [
            pltpu.make_async_copy(gn, gain_v.at[s], load_sem.at[4 * s + 1]),
            pltpu.make_async_copy(gt, gate_v.at[s], load_sem.at[4 * s + 2]),
            pltpu.make_async_copy(up, up_v.at[s], load_sem.at[4 * s + 3]),
            pltpu.make_async_copy(dn, down_v.at[s], load_sem.at[4 * s + 4]),
        ]
    for c in loads:
        c.start()

    turn = lax.rem(ra + n_ra - 1, n_ra)
    odd = lax.rem(cb, 2) == 1
    partner = {"cb": cb + 1 - 2 * lax.rem(cb, 2)}

    def later(o):
        return turn + o < n_ra

    barrier = pltpu.get_barrier_semaphore()

    @pl.when(turn == 0)
    def _():
        for o in range(1, n_cb):
            pl.semaphore_signal(barrier, 1, device_id={"cb": lax.rem(cb + o, n_cb)}, device_id_type=MESH)

    @pl.when(jnp.logical_and(turn > 0, jnp.logical_not(odd)))
    def _():
        pl.semaphore_signal(barrier, 1, device_id=partner, device_id_type=MESH)

    with scope("barrier"):
        pl.semaphore_wait(barrier, jnp.where(turn == 0, n_cb - 1, jnp.where(odd, 2, 1)))

    @pl.when(jnp.logical_and(turn < n_ra - 1, odd))
    def _():
        pl.semaphore_signal(barrier, 1, device_id={"ra": lax.rem(ra + 1, n_ra)}, device_id_type=MESH)

    @pl.when(jnp.logical_and(turn > 0, odd))
    def _():
        pl.semaphore_signal(barrier, 1, device_id=partner, device_id_type=MESH)

    for o in near:
        @pl.when(turn >= o)
        def _():
            pl.semaphore_signal(ready.at[near.index(o)], 1, device_id={"ra": at(n_ra - o)}, device_id_type=MESH)

    @pl.when(turn > 0)
    def _():
        pl.semaphore_signal(column, 1, device_id={"ra": lax.rem(ra + n_ra - turn, n_ra)}, device_id_type=MESH)

    def project(s, xf, places):
        sq = jnp.sum(xf * xf, axis=1, keepdims=True)
        normed = (xf * gain_v[s].astype(F32)).astype(BF16)
        gate, up = (
            lax.dot_general(normed, w[s], (((1,), (1,)), ((), ())), preferred_element_type=F32)
            for w in (gate_v, up_v))
        ends = jnp.concatenate([gate[:, main:], up[:, main:]], axis=1)
        for i, place in enumerate(places):
            cut = slice(i * piece, (i + 1) * piece)
            rs_out[s, place, :, :main] = gate[cut, :main].astype(BF16)
            rs_out[s, place, :, main:2 * main] = up[cut, :main].astype(BF16)
            rs_out[s, place, :, 2 * main:2 * units] = ends[cut].astype(BF16)
            sq_out[s, place] = jnp.sum(jnp.where(diagonal, sq[cut], 0.0), axis=0, keepdims=True)

    def batch(o):
        return 0 if o in ahead else 1 if o in behind else 2 if o == hop else 3 if o == n_ra - hop else 4

    def all_of(ref, send_sem, recv_sem):
        return pltpu.make_async_remote_copy(
            src_ref=ref, dst_ref=ref, send_sem=send_sem, recv_sem=recv_sem,
            device_id={"ra": at(1)}, device_id_type=MESH)

    def scattered(s, count, which=0):
        return (
            all_of(rs_in.at[s, pl.ds(0, count)], rs_send.at[s], rs_recv.at[s, which]),
            all_of(sq_in.at[s, pl.ds(0, count)], sq_send.at[s], sq_recv.at[s, which]))

    def arrived(s, count, which):
        for c in scattered(s, count, which):
            c.wait_recv()

    def scatter(s):
        def ring(src, src_sq, o, to):
            both = [
                pltpu.make_async_remote_copy(
                    src_ref=ref, dst_ref=dst.at[s, o], send_sem=send.at[s], recv_sem=recv.at[s, batch(o)],
                    device_id={"ra": at(to)}, device_id_type=MESH)
                for ref, dst, send, recv in (
                    (src_sq, sq_in, sq_send, sq_recv), (src, rs_in, rs_send, rs_recv))]

            def start():
                for c in both:
                    c.start()

            return start

        def term(o, to):
            return ring(rs_out.at[s, at(o)], sq_out.at[s, at(o)], o, to)

        copies = {o: term(o, o) for o in near if o not in relays}
        copies |= {o: term(o, o - hop) for o in ahead}
        copies |= {o: term(o, o + hop) for o in behind}
        copies |= {o: ring(sums.at[s, i], sq_sums.at[s, i], o, o) for i, o in enumerate(relays)}
        return copies

    def via(o):
        return o - hop if o in ahead else o + hop if o in behind else o

    def ag_copy(s, o):
        seen = n_ra - o
        group = [seen in g for g in all_groups[s]].index(True)
        return pltpu.make_async_remote_copy(
            src_ref=ag_out.at[s], dst_ref=ag_in.at[s, ra], send_sem=ag_send.at[s],
            recv_sem=ag_recv.at[s, group], device_id={"ra": at(o)}, device_id_type=MESH)

    def gathered(s, count, recv_sem):
        return all_of(ag_in.at[s, pl.ds(0, count)], ag_send.at[s], recv_sem)

    def summed(s, g):
        return all_of(ar_ins[s].at[g, pl.ds(0, n_cb - 1)], ar_send.at[s, g], ar_recv.at[s, g])

    rs = [scatter(s) for s in range(2)]
    free = [o for o in far_first(n_ra) if o not in relays]

    with scope("load"):
        for c in loads[:4]:
            c.wait()
    with scope("project_first"):
        xf = x_v[...].astype(F32)
        for i in range(n_ra):
            x_f[i] = xf[i * piece:(i + 1) * piece]
        project(0, xf, range(n_ra))
    with scope("send_first"):
        for o in free:
            pl.when(jnp.logical_not(later(via(o))))(rs[0][o])
    with scope("send_ready"):
        for p in near:
            @pl.when(later(p))
            def _():
                pl.semaphore_wait(ready.at[near.index(p)], 1)
                for o in free:
                    if via(o) == p:
                        rs[0][o]()

    @pl.when(turn == 0)
    def _():
        pl.semaphore_wait(column, n_ra - 1)
        for o in range(1, n_cb):
            pl.semaphore_signal(row, 1, device_id={"cb": lax.rem(cb + o, n_cb)}, device_id_type=MESH)
        pl.semaphore_wait(row, n_cb - 1)
        for o in far_first(n_ra):
            pl.semaphore_signal(all_in, 1, device_id={"ra": at(o)}, device_id_type=MESH)

    for s in range(2):
        for i, (o, far) in enumerate(zip(relays, (behind, ahead))):
            part = rs_out[s, at(o)].astype(F32)
            with scope(f"relay_wait{s}_{o}"):
                arrived(s, len(far), batch(far[0]))
            part_sq = sq_out[s, at(o)]
            for f in far:
                part = part + rs_in[s, f].astype(F32)
                part_sq = part_sq + sq_in[s, f]
            sums[s, i] = part.astype(BF16)
            sq_sums[s, i] = part_sq
            rs[s][o]()
        total = rs_out[s, ra].astype(F32)
        direct = [o for o in near if o not in relays]
        with scope(f"scatter_wait{s}_direct"):
            arrived(s, len(direct), batch(direct[0]))
        total_sq = sq_out[s, ra]
        for o in direct:
            total = total + rs_in[s, o].astype(F32)
            total_sq = total_sq + sq_in[s, o]
        for o in relays:
            with scope(f"scatter_wait{s}_{o}"):
                arrived(s, 1, batch(o))
            total = total + rs_in[s, o].astype(F32)
            total_sq = total_sq + sq_in[s, o]
        sumsq = jnp.sum(jnp.where(diagonal, total_sq, 0.0), axis=1, keepdims=True)
        scale = lax.rsqrt(sumsq / width + 1e-06)
        ends = total[:, 2 * main:2 * units]
        g = jnp.concatenate([total[:, :main], ends[:, :rest]], axis=1) * scale
        u = jnp.concatenate([total[:, main:2 * main], ends[:, rest:]], axis=1) * scale
        hidden = (g / (1.0 + jnp.exp(-g)) * u).astype(BF16)
        ag_out[s] = hidden
        ag_in[s, ra] = hidden
        ag = [ag_copy(s, o) for o in far_first(n_ra)]
        if s == 1:
            for tier in range(4):
                for o, c in zip(far_first(n_ra), ag):
                    pl.when(at(o) // (n_ra // 4) == tier)(c.start)
        else:
            for c in ag:
                c.start()
        loads[4 * s + 4].wait()
        for c in scattered(s, n_ra - 1):
            c.wait_send()
        if s == 0:
            for c in loads[5:8]:
                c.wait()

        groups = all_groups[s]
        ar_in = ar_ins[s]

        def down(g):
            with scope(f"gather_wait{s}_{g}"):
                count = sum(o != 0 for o in groups[g])
                gathered(s, count, ag_recv.at[s, g]).wait_recv()
            h = jnp.concatenate([ag_in[s, at(o)].astype(F32) for o in groups[g]], axis=0).astype(BF16)
            ar_in[g, cb] = jnp.dot(h, down_v[s], preferred_element_type=F32).astype(BF16)
            for o in far_first(n_cb):
                pltpu.make_async_remote_copy(
                    src_ref=ar_in.at[g, cb], dst_ref=ar_in.at[g, cb], send_sem=ar_send.at[s, g],
                    recv_sem=ar_recv.at[s, g], device_id={"cb": lax.rem(cb + o, n_cb)}, device_id_type=MESH).start()

        def finish(g):
            with scope(f"cb_wait{s}_{g}"):
                summed(s, g).wait_recv()
            branch = ar_in[g, 0].astype(F32)
            for c in range(1, n_cb):
                branch = branch + ar_in[g, c].astype(F32)
            places = [at(o) for o in groups[g]]
            old = jnp.concatenate([x_f[p] for p in places], axis=0)
            result = (0.5 * old + 0.5 * branch).astype(BF16)
            if s == 1:
                for i, p in enumerate(places):
                    out[p] = result[i * piece:(i + 1) * piece]
                return
            new = result.astype(F32)
            for i, p in enumerate(places):
                x_f[p] = new[i * piece:(i + 1) * piece]
            project(1, new, places)
            for o in groups[g]:
                if o in free:
                    rs[1][o]()

        if s == 0:
            with scope("all_in"):
                @pl.when(turn > 0)
                def _():
                    pl.semaphore_wait(all_in, 1)
        for g in range(len(groups)):
            down(g)
        gathered(s, n_ra - 1, ag_recv.at[s, 0]).wait_send()
        for g in range(len(groups)):
            finish(g)
        for g in range(len(groups)):
            summed(s, g).wait_send()


def per_device(tokens, first_gain, first_gate, first_up, first_down,
               second_gain, second_gate, second_up, second_down):
    n_ra, n_cb = lax.axis_size("ra"), lax.axis_size("cb")
    rows, cols = tokens.shape
    units = first_gate.shape[1]
    piece = rows // n_ra
    dma = pltpu.SemaphoreType.DMA
    any_spec = pl.BlockSpec(memory_space=pl.ANY)
    out = pl.pallas_call(
        functools.partial(fused, n_ra, n_cb),
        out_shape=pltpu.VMEM((n_ra, piece, cols), BF16),
        in_specs=[any_spec] * 9,
        out_specs=pl.BlockSpec(memory_space=pltpu.VMEM),
        scratch_shapes=[
            pltpu.VMEM((rows, cols), BF16),
            pltpu.VMEM((2, 1, cols), BF16),
            pltpu.VMEM((2, units, cols), BF16),
            pltpu.VMEM((2, units, cols), BF16),
            pltpu.VMEM((2, units, cols), BF16),
            pltpu.VMEM((n_ra, piece, cols), F32),
            pltpu.VMEM((2, n_ra, piece, 2 * units), BF16),
            pltpu.VMEM((2, 2, piece, 2 * units), BF16),
            pltpu.VMEM((2, n_ra, piece, 2 * units), BF16),
            pltpu.VMEM((2, n_ra, 1, LANES), F32),
            pltpu.VMEM((2, 2, 1, LANES), F32),
            pltpu.VMEM((2, n_ra, 1, LANES), F32),
            pltpu.VMEM((2, piece, units), BF16),
            pltpu.VMEM((2, n_ra, piece, units), BF16),
            *(pltpu.VMEM((k, n_cb, rows // k, cols), BF16) for k in GROUPS),
            pltpu.SemaphoreType.REGULAR((n_ra // 2,)),
            pltpu.SemaphoreType.REGULAR,
            pltpu.SemaphoreType.REGULAR,
            pltpu.SemaphoreType.REGULAR,
            dma((9,)),
            dma((2,)), dma((2, 5)), dma((2,)), dma((2, 5)),
            dma((2,)), dma((2, max(GROUPS))),
            dma((2, max(GROUPS))), dma((2, max(GROUPS))),
        ],
        compiler_params=pltpu.CompilerParams(collective_id=0, has_side_effects=True),
    )(tokens, first_gain.reshape(1, -1), first_gate.T, first_up.T, first_down,
      second_gain.reshape(1, -1), second_gate.T, second_up.T, second_down)
    return out.reshape(rows, cols)


def solution(mesh):
    placed = (
        P("grp", "ra"),
        P("ra"), P("ra", "cb"), P("ra", "cb"), P("cb", "ra"),
        P("ra"), P("ra", "cb"), P("ra", "cb"), P("cb", "ra"),
    )
    return jax.shard_map(
        per_device, mesh=mesh, in_specs=placed, out_specs=P("grp", "ra"), check_vma=False
    )
```

```python
import functools

import jax
import jax.numpy as jnp
from jax import lax
from jax.experimental import pallas as pl
from jax.experimental.pallas import tpu as pltpu
from jax.sharding import PartitionSpec as P

MESH = pl.DeviceIdType.MESH
LANES = 128
BF16 = jnp.bfloat16
F32 = jnp.float32
scope = jax.named_scope
GROUPS = (8, 4)


def far_first(n):
    return sorted(range(1, n), key=lambda o: -min(o, n - o))


def groups_of(n):
    order = far_first(n) + [0]
    return [[order[i:i + n // k] for i in range(0, n, n // k)] for k in GROUPS]


def fused(n_ra, n_cb, tokens, gain1, gate1, up1, down1, gain2, gate2, up2, down2, out,
          x_v, gain_v, gate_v, up_v, down_v, x_f,
          rs_out, sums, rs_in, sq_out, sq_sums, sq_in, ag_out, ag_in, ar_in1, ar_in2,
          ready, column, row, all_in, load_sem, rs_send, rs_recv, sq_send, sq_recv, ag_send, ag_recv, ar_send, ar_recv):
    ra = lax.axis_index("ra")
    cb = lax.axis_index("cb")
    rows, cols = x_v.shape
    piece = rows // n_ra
    units = gate_v.shape[1]
    main = units // LANES * LANES
    rest = units - main
    diagonal = lax.broadcasted_iota(jnp.int32, (piece, LANES), 0) == lax.broadcasted_iota(jnp.int32, (piece, LANES), 1)
    width = cols * n_ra
    ar_ins = (ar_in1, ar_in2)
    all_groups = groups_of(n_ra)

    hop = n_ra // 4
    ahead = list(range(hop + 1, n_ra // 2 + 1))
    behind = list(range(n_ra // 2 + 1, n_ra - hop))
    near = list(range(1, hop + 1)) + list(range(n_ra - hop, n_ra))

    relays = (n_ra - hop, hop)

    def at(o):
        return lax.rem(ra + o, n_ra)

    loads = [pltpu.make_async_copy(tokens, x_v, load_sem.at[0])]
    for s, (gn, gt, up, dn) in enumerate(((gain1, gate1, up1, down1), (gain2, gate2, up2, down2))):
        loads += [
            pltpu.make_async_copy(gn, gain_v.at[s], load_sem.at[4 * s + 1]),
            pltpu.make_async_copy(gt, gate_v.at[s], load_sem.at[4 * s + 2]),
            pltpu.make_async_copy(up, up_v.at[s], load_sem.at[4 * s + 3]),
            pltpu.make_async_copy(dn, down_v.at[s], load_sem.at[4 * s + 4]),
        ]
    for c in loads:
        c.start()

    turn = lax.rem(ra + n_ra - 1, n_ra)
    odd = lax.rem(cb, 2) == 1
    partner = {"cb": cb + 1 - 2 * lax.rem(cb, 2)}

    def later(o):
        return turn + o < n_ra

    barrier = pltpu.get_barrier_semaphore()

    @pl.when(turn == 0)
    def _():
        for o in range(1, n_cb):
            pl.semaphore_signal(barrier, 1, device_id={"cb": lax.rem(cb + o, n_cb)}, device_id_type=MESH)

    @pl.when(jnp.logical_and(turn > 0, jnp.logical_not(odd)))
    def _():
        pl.semaphore_signal(barrier, 1, device_id=partner, device_id_type=MESH)

    with scope("barrier"):
        pl.semaphore_wait(barrier, jnp.where(turn == 0, n_cb - 1, jnp.where(odd, 2, 1)))

    @pl.when(jnp.logical_and(turn < n_ra - 1, odd))
    def _():
        pl.semaphore_signal(barrier, 1, device_id={"ra": lax.rem(ra + 1, n_ra)}, device_id_type=MESH)

    @pl.when(jnp.logical_and(turn > 0, odd))
    def _():
        pl.semaphore_signal(barrier, 1, device_id=partner, device_id_type=MESH)

    for o in near:
        @pl.when(turn >= o)
        def _():
            pl.semaphore_signal(ready.at[near.index(o)], 1, device_id={"ra": at(n_ra - o)}, device_id_type=MESH)

    @pl.when(turn > 0)
    def _():
        pl.semaphore_signal(column, 1, device_id={"ra": lax.rem(ra + n_ra - turn, n_ra)}, device_id_type=MESH)

    def project(s, xf, places):
        sq = jnp.sum(xf * xf, axis=1, keepdims=True)
        normed = (xf * gain_v[s].astype(F32)).astype(BF16)
        gate, up = (
            lax.dot_general(normed, w[s], (((1,), (1,)), ((), ())), preferred_element_type=F32)
            for w in (gate_v, up_v))
        ends = jnp.concatenate([gate[:, main:], up[:, main:]], axis=1)
        for i, place in enumerate(places):
            cut = slice(i * piece, (i + 1) * piece)
            rs_out[s, place, :, :main] = gate[cut, :main].astype(BF16)
            rs_out[s, place, :, main:2 * main] = up[cut, :main].astype(BF16)
            rs_out[s, place, :, 2 * main:2 * units] = ends[cut].astype(BF16)
            sq_out[s, place] = jnp.sum(jnp.where(diagonal, sq[cut], 0.0), axis=0, keepdims=True)

    def batch(o):
        return 0 if o in ahead else 1 if o in behind else 2 if o in relays else 3

    def all_of(ref, send_sem, recv_sem):
        return pltpu.make_async_remote_copy(
            src_ref=ref, dst_ref=ref, send_sem=send_sem, recv_sem=recv_sem,
            device_id={"ra": at(1)}, device_id_type=MESH)

    def scattered(s, count, which=0):
        return (
            all_of(rs_in.at[s, pl.ds(0, count)], rs_send.at[s], rs_recv.at[s, which]),
            all_of(sq_in.at[s, pl.ds(0, count)], sq_send.at[s], sq_recv.at[s, which]))

    def arrived(s, count, which):
        for c in scattered(s, count, which):
            c.wait_recv()

    def scatter(s):
        def ring(src, src_sq, o, to):
            both = [
                pltpu.make_async_remote_copy(
                    src_ref=ref, dst_ref=dst.at[s, o], send_sem=send.at[s], recv_sem=recv.at[s, batch(o)],
                    device_id={"ra": at(to)}, device_id_type=MESH)
                for ref, dst, send, recv in (
                    (src_sq, sq_in, sq_send, sq_recv), (src, rs_in, rs_send, rs_recv))]

            def start():
                for c in both:
                    c.start()

            return start

        def term(o, to):
            return ring(rs_out.at[s, at(o)], sq_out.at[s, at(o)], o, to)

        copies = {o: term(o, o) for o in near if o not in relays}
        copies |= {o: term(o, o - hop) for o in ahead}
        copies |= {o: term(o, o + hop) for o in behind}
        copies |= {o: ring(sums.at[s, i], sq_sums.at[s, i], o, o) for i, o in enumerate(relays)}
        return copies

    def via(o):
        return o - hop if o in ahead else o + hop if o in behind else o

    def ag_copy(s, o):
        seen = n_ra - o
        group = [seen in g for g in all_groups[s]].index(True)
        return pltpu.make_async_remote_copy(
            src_ref=ag_out.at[s], dst_ref=ag_in.at[s, ra], send_sem=ag_send.at[s],
            recv_sem=ag_recv.at[s * GROUPS[0] + group], device_id={"ra": at(o)}, device_id_type=MESH)

    def gathered(s, count, recv_sem):
        return all_of(ag_in.at[s, pl.ds(0, count)], ag_send.at[s], recv_sem)

    def summed(s, g):
        return all_of(ar_ins[s].at[g, pl.ds(0, n_cb - 1)], ar_send.at[s], ar_recv.at[s * GROUPS[0] + g])

    rs = [scatter(s) for s in range(2)]
    free = [o for o in far_first(n_ra) if o not in relays]

    with scope("load"):
        for c in loads[:4]:
            c.wait()
    with scope("project_first"):
        xf = x_v[...].astype(F32)
        for i in range(n_ra):
            x_f[i] = xf[i * piece:(i + 1) * piece]
        project(0, xf, range(n_ra))
    with scope("send_first"):
        for o in free:
            pl.when(jnp.logical_not(later(via(o))))(rs[0][o])
    with scope("send_ready"):
        for p in near:
            @pl.when(later(p))
            def _():
                pl.semaphore_wait(ready.at[near.index(p)], 1)
                for o in free:
                    if via(o) == p:
                        rs[0][o]()

    @pl.when(turn == 0)
    def _():
        pl.semaphore_wait(column, n_ra - 1)
        for o in range(1, n_cb):
            pl.semaphore_signal(row, 1, device_id={"cb": lax.rem(cb + o, n_cb)}, device_id_type=MESH)
        pl.semaphore_wait(row, n_cb - 1)
        for o in far_first(n_ra):
            pl.semaphore_signal(all_in, 1, device_id={"ra": at(o)}, device_id_type=MESH)

    for s in range(2):
        for i, (o, far) in enumerate(zip(relays, (behind, ahead))):
            part = rs_out[s, at(o)].astype(F32)
            with scope(f"relay_wait{s}_{o}"):
                arrived(s, len(far), batch(far[0]))
            part_sq = sq_out[s, at(o)]
            for f in far:
                part = part + rs_in[s, f].astype(F32)
                part_sq = part_sq + sq_in[s, f]
            sums[s, i] = part.astype(BF16)
            sq_sums[s, i] = part_sq
            rs[s][o]()
        total = rs_out[s, ra].astype(F32)
        direct = [o for o in near if o not in relays]
        with scope(f"scatter_wait{s}_direct"):
            arrived(s, len(direct), batch(direct[0]))
        total_sq = sq_out[s, ra]
        for o in direct:
            total = total + rs_in[s, o].astype(F32)
            total_sq = total_sq + sq_in[s, o]
        with scope(f"scatter_wait{s}_relays"):
            arrived(s, len(relays), batch(hop))
        for o in relays:
            total = total + rs_in[s, o].astype(F32)
            total_sq = total_sq + sq_in[s, o]
        sumsq = jnp.sum(jnp.where(diagonal, total_sq, 0.0), axis=1, keepdims=True)
        scale = lax.rsqrt(sumsq / width + 1e-06)
        ends = total[:, 2 * main:2 * units]
        g = jnp.concatenate([total[:, :main], ends[:, :rest]], axis=1) * scale
        u = jnp.concatenate([total[:, main:2 * main], ends[:, rest:]], axis=1) * scale
        hidden = (g / (1.0 + jnp.exp(-g)) * u).astype(BF16)
        ag_out[s] = hidden
        ag_in[s, ra] = hidden
        ag = [ag_copy(s, o) for o in far_first(n_ra)]
        if s == 1:
            for tier in range(4):
                for o, c in zip(far_first(n_ra), ag):
                    pl.when(at(o) // (n_ra // 4) == tier)(c.start)
        else:
            for c in ag:
                c.start()
        loads[4 * s + 4].wait()
        for c in scattered(s, n_ra - 1):
            c.wait_send()
        if s == 0:
            for c in loads[5:8]:
                c.wait()

        groups = all_groups[s]
        ar_in = ar_ins[s]

        def down(g):
            with scope(f"gather_wait{s}_{g}"):
                count = sum(o != 0 for o in groups[g])
                gathered(s, count, ag_recv.at[s * GROUPS[0] + g]).wait_recv()
            h = jnp.concatenate([ag_in[s, at(o)].astype(F32) for o in groups[g]], axis=0).astype(BF16)
            ar_in[g, cb] = jnp.dot(h, down_v[s], preferred_element_type=F32).astype(BF16)
            for o in far_first(n_cb):
                pltpu.make_async_remote_copy(
                    src_ref=ar_in.at[g, cb], dst_ref=ar_in.at[g, cb], send_sem=ar_send.at[s],
                    recv_sem=ar_recv.at[s * GROUPS[0] + g], device_id={"cb": lax.rem(cb + o, n_cb)}, device_id_type=MESH).start()

        def finish(g):
            with scope(f"cb_wait{s}_{g}"):
                summed(s, g).wait_recv()
            branch = ar_in[g, 0].astype(F32)
            for c in range(1, n_cb):
                branch = branch + ar_in[g, c].astype(F32)
            places = [at(o) for o in groups[g]]
            old = jnp.concatenate([x_f[p] for p in places], axis=0)
            result = (0.5 * old + 0.5 * branch).astype(BF16)
            if s == 1:
                for i, p in enumerate(places):
                    out[p] = result[i * piece:(i + 1) * piece]
                return
            new = result.astype(F32)
            for i, p in enumerate(places):
                x_f[p] = new[i * piece:(i + 1) * piece]
            project(1, new, places)
            for o in groups[g]:
                if o in free:
                    rs[1][o]()

        if s == 0:
            with scope("all_in"):
                @pl.when(turn > 0)
                def _():
                    pl.semaphore_wait(all_in, 1)
        for g in range(len(groups)):
            down(g)
        gathered(s, n_ra - 1, ag_recv.at[s * GROUPS[0]]).wait_send()
        for g in range(len(groups)):
            finish(g)
        all_of(ar_in.at[pl.ds(0, len(groups)), pl.ds(0, n_cb - 1)], ar_send.at[s], ar_recv.at[0]).wait_send()


def per_device(tokens, first_gain, first_gate, first_up, first_down,
               second_gain, second_gate, second_up, second_down):
    n_ra, n_cb = lax.axis_size("ra"), lax.axis_size("cb")
    rows, cols = tokens.shape
    units = first_gate.shape[1]
    piece = rows // n_ra
    dma = pltpu.SemaphoreType.DMA
    any_spec = pl.BlockSpec(memory_space=pl.ANY)
    out = pl.pallas_call(
        functools.partial(fused, n_ra, n_cb),
        out_shape=pltpu.VMEM((n_ra, piece, cols), BF16),
        in_specs=[any_spec] * 9,
        out_specs=pl.BlockSpec(memory_space=pltpu.VMEM),
        scratch_shapes=[
            pltpu.VMEM((rows, cols), BF16),
            pltpu.VMEM((2, 1, cols), BF16),
            pltpu.VMEM((2, units, cols), BF16),
            pltpu.VMEM((2, units, cols), BF16),
            pltpu.VMEM((2, units, cols), BF16),
            pltpu.VMEM((n_ra, piece, cols), F32),
            pltpu.VMEM((2, n_ra, piece, 2 * units), BF16),
            pltpu.VMEM((2, 2, piece, 2 * units), BF16),
            pltpu.VMEM((2, n_ra, piece, 2 * units), BF16),
            pltpu.VMEM((2, n_ra, 1, LANES), F32),
            pltpu.VMEM((2, 2, 1, LANES), F32),
            pltpu.VMEM((2, n_ra, 1, LANES), F32),
            pltpu.VMEM((2, piece, units), BF16),
            pltpu.VMEM((2, n_ra, piece, units), BF16),
            *(pltpu.VMEM((k, n_cb, rows // k, cols), BF16) for k in GROUPS),
            pltpu.SemaphoreType.REGULAR((n_ra // 2,)),
            pltpu.SemaphoreType.REGULAR,
            pltpu.SemaphoreType.REGULAR,
            pltpu.SemaphoreType.REGULAR,
            dma((9,)),
            dma((2,)), dma((2, 4)), dma((2,)), dma((2, 4)),
            dma((2,)), dma((sum(GROUPS),)),
            dma((2,)), dma((sum(GROUPS),)),
        ],
        compiler_params=pltpu.CompilerParams(collective_id=0, has_side_effects=True),
    )(tokens, first_gain.reshape(1, -1), first_gate.T, first_up.T, first_down,
      second_gain.reshape(1, -1), second_gate.T, second_up.T, second_down)
    return out.reshape(rows, cols)


def solution(mesh):
    placed = (
        P("grp", "ra"),
        P("ra"), P("ra", "cb"), P("ra", "cb"), P("cb", "ra"),
        P("ra"), P("ra", "cb"), P("ra", "cb"), P("cb", "ra"),
    )
    return jax.shard_map(
        per_device, mesh=mesh, in_specs=placed, out_specs=P("grp", "ra"), check_vma=False
    )
```
